32 devices in a mesh: sp: 8 (over z, y), tp: 4 (over x, core).
Axes of the slice: x: 2, y: 2, z: 4, core: 2. Of those that a mesh axis runs over, the one named last changes fastest.
Arguments:
- tokens: bfloat16 [8192, 2048], P(('sp', 'tp')), may hold values from -6 to 6
- norm_gain: float32 [2048], replicated, may hold values from 0.1 to 1.9
- w_query: bfloat16 [2048, 2048], P(None, 'tp'), may hold values from -0.125 to 0.125
- w_forget: bfloat16 [2048, 2048], P(None, 'tp'), may hold values from -0.125 to 0.125
- w_value: bfloat16 [2048, 2048], P(None, 'tp'), may hold values from -0.125 to 0.125
- w_rgate: bfloat16 [2048, 2048], P(None, 'tp'), may hold values from -0.125 to 0.125
- w_glu_value: bfloat16 [2048, 2048], P(None, 'tp'), may hold values from -0.125 to 0.125
- w_glu_gate: bfloat16 [2048, 2048], P(None, 'tp'), may hold values from -0.125 to 0.125
- forget_gap: float32 [2048], P('tp'), may hold values from 6.1035156e-05 to 0.1
- decay_shift: float32 [8192, 16], P('sp', 'tp'), may hold values from -0.6 to 0, as said below
- head_gain: float32 [128], replicated, may hold values from 0.1 to 1.9
- conv_taps: float32 [31, 2048], P(None, 'tp'), may hold values from -12 to 12
- conv_gain: float32 [2048], P('tp'), may hold values from 0.1 to 1.9
- out_rec: bfloat16 [2048, 2048], P('tp'), may hold values from -0.09375 to 0.09375
- out_conv: bfloat16 [2048, 2048], P('tp'), may hold values from -0.09375 to 0.09375
Outputs:
- mixed: bfloat16 [8192, 2048], P(('sp', 'tp'))
The draws below stay inside these ranges and needn't reach their ends.
Inputs may be any that keep to these rules, and one draw needn't show every extreme that they name: `decay_shift`: at most zero everywhere.
All inputs are finite; a program needn't handle non-finite values.
Results may differ from the reference program's by a relative error of at most 0.015.
Values may be sent and summed in bfloat16 or wider, within the bound.
A program may use at most 128 MiB of HBM per device.

```python
import jax
import jax.numpy as jnp
from jax import lax

D = 2048
HEADS = 16
HEAD = 128
DC = 2048
CW = 31
BLOCK = 64
TOK_DEV = 1024
DH = 2048
TOKENS = 8192
N_TP = 4


def draw_forget_gap(key, part):
    order = jax.random.permutation(jax.random.fold_in(key, 3), HEADS)
    fast_count = HEADS // 2
    fast = order < fast_count
    spread = jax.random.uniform(jax.random.fold_in(key, 5), (HEADS, HEAD), jnp.float32)
    slow_gap = jnp.exp(jnp.log(0.5) + spread * jnp.log(3.0)) / TOKENS
    fast_gap = jnp.exp(jnp.log(0.03) + spread * jnp.log(10.0 / 3.0))
    return jnp.where(fast[:, None], fast_gap, slow_gap).reshape(HEADS * HEAD)


def draw_decay_shift(key, part):
    block_total = TOKENS // TOK_DEV
    spread = jax.random.uniform(jax.random.fold_in(key, 7), (block_total, 1), jnp.float32)
    rate = jnp.exp(jnp.log(0.2) + spread * jnp.log(5.0)) / TOKENS
    smooth_part = -jnp.repeat(rate, TOK_DEV, axis=0) * jnp.ones((1, HEADS), jnp.float32)
    positions = jax.random.randint(jax.random.fold_in(key, 11), (2,), 0, TOKENS)
    depth = jax.random.uniform(jax.random.fold_in(key, 13), (2, HEADS), jnp.float32, 0.2, 0.4)
    hits = (jnp.arange(TOKENS)[:, None] == positions[None, :]).astype(jnp.float32)
    return smooth_part + jnp.dot(hits, jnp.log(1.0 - depth))


def draw_conv_taps(key, part):
    channel_rise = jnp.exp(jnp.log(3.0) * jnp.arange(DC).astype(jnp.float32) / DC)
    base = jnp.clip(jax.random.normal(jax.random.fold_in(key, 17), (CW, DC), jnp.float32), -4.0, 4.0)
    spread = jnp.exp(jax.random.uniform(jax.random.fold_in(key, 19), (DC,), jnp.float32, 0.0, jnp.log(10.0)))
    scale = 0.1
    return base * channel_rise * spread * scale


def levels(rng, shape, split, least, top_value):
    factor_of = 1.0
    for dim, blocks in split:
        steps = jax.random.uniform(jax.random.fold_in(jax.random.fold_in(rng, 6), dim), (blocks,), jnp.float32, least / len(split), top_value / len(split))
        factor_of = factor_of * jnp.repeat(jnp.exp(steps), shape[dim] // blocks).reshape((-1,) + (1,) * (len(shape) - 1 - dim))
    return factor_of


def gaussian(rng, dims, scale, most, split=(), kind=jnp.bfloat16):
    level = levels(rng, dims, split, -0.22, 0.18) if split else 1.0
    values = jax.random.normal(rng, dims, jnp.float32) * scale * level
    return jnp.minimum(jnp.maximum(values, -most), most).astype(kind)


def setup_inputs(seed: int = 0) -> dict:
    streams_of = jax.random.split(jax.random.key(seed), 16)
    tokens = gaussian(streams_of[0], (TOKENS, D), 1.0, 6.0, ((0, 32),))
    norm_gain = jnp.clip(1.0 + 0.18 * jax.random.normal(streams_of[1], (D,), jnp.float32), 0.1, 1.9)
    w_query = gaussian(streams_of[2], (D, DH), D ** -0.5, 0.125, ((1, 4),))
    w_forget = gaussian(streams_of[3], (D, DH), D ** -0.5, 0.125, ((1, 4),))
    w_value = gaussian(streams_of[4], (D, DH), D ** -0.5, 0.125, ((1, 4),))
    w_rgate = gaussian(streams_of[5], (D, DH), D ** -0.5, 0.125, ((1, 4),))
    w_glu_value = gaussian(streams_of[6], (D, DC), D ** -0.5, 0.125, ((1, 4),))
    w_glu_gate = gaussian(streams_of[7], (D, DC), D ** -0.5, 0.125, ((1, 4),))
    forget_gap = draw_forget_gap(jax.random.fold_in(streams_of[15], 71), 0)
    decay_shift = draw_decay_shift(jax.random.fold_in(streams_of[15], 71), 0)
    head_gain = jnp.clip(1.0 + 0.18 * jax.random.normal(streams_of[10], (HEAD,), jnp.float32), 0.1, 1.9)
    conv_taps = draw_conv_taps(jax.random.fold_in(streams_of[15], 71), 0)
    conv_gain = jnp.clip(1.0 + 0.18 * jax.random.normal(streams_of[12], (DC,), jnp.float32), 0.1, 1.9)
    out_rec = gaussian(streams_of[13], (DH, D), (DH + DC) ** -0.5, 0.09375, ((0, 4),))
    out_conv = gaussian(streams_of[14], (DC, D), (DH + DC) ** -0.5, 0.09375, ((0, 4),))
    return {"tokens": tokens, "norm_gain": norm_gain, "w_query": w_query, "w_forget": w_forget, "w_value": w_value, "w_rgate": w_rgate, "w_glu_value": w_glu_value, "w_glu_gate": w_glu_gate, "forget_gap": forget_gap, "decay_shift": decay_shift, "head_gain": head_gain, "conv_taps": conv_taps, "conv_gain": conv_gain, "out_rec": out_rec, "out_conv": out_conv}


precise_setting = lax.Precision.HIGHEST
norm_epsilon = 1e-05
head_epsilon = 1e-06

def layer_norm(values, gain):
    widened = values.astype(jnp.float32)
    row_mean = lax.optimization_barrier(jnp.mean(widened, axis=-1, keepdims=True))
    centred = widened - row_mean
    row_var = lax.optimization_barrier(jnp.mean(centred * centred, axis=-1, keepdims=True))
    return centred * lax.rsqrt(row_var + norm_epsilon) * gain.astype(jnp.float32)

def block_scan(query, key_gate, values, log_forget):
    row_count, head_count, key_width = query.shape
    value_width = values.shape[2]
    block_count = row_count // BLOCK

    def to_blocks(array):
        return array.reshape(block_count, BLOCK, head_count, array.shape[2]).transpose(0, 2, 1, 3)
    causal = lax.broadcasted_iota(jnp.int32, (BLOCK, BLOCK), 0) >= lax.broadcasted_iota(jnp.int32, (BLOCK, BLOCK), 1)

    def advance(current_state, inputs):
        query_blk, key_block, value_block, log_blk = inputs
        running_total = jnp.cumsum(log_blk, axis=1)
        closing_log = running_total[:, -1:, :]
        query_decayed = query_blk * jnp.exp(running_total)
        scores = jnp.einsum('htk,hsk->hts', query_decayed, key_block * jnp.exp(-running_total), precision=precise_setting)
        scores = jnp.where(causal[None], scores, 0.0)
        output_rows = jnp.einsum('hts,hsv->htv', scores, value_block, precision=precise_setting)
        output_rows = output_rows + jnp.einsum('ori,oiq->orq', query_decayed, current_state, precision=precise_setting)
        current_state = jnp.exp(closing_log[:, 0, :])[:, :, None] * current_state + jnp.einsum('itp,ito->ipo', key_block * jnp.exp(closing_log - running_total), value_block, precision=precise_setting)
        return (current_state, output_rows)
    start_state = jnp.zeros((head_count, key_width, value_width), jnp.float32)
    final_state, output_rows = lax.scan(advance, start_state, (to_blocks(query), to_blocks(key_gate), to_blocks(values), to_blocks(log_forget)))
    return output_rows.transpose(0, 2, 1, 3).reshape(row_count, head_count, value_width)

def reference(tokens, norm_gain, w_query, w_forget, w_value, w_rgate, w_glu_value, w_glu_gate, forget_gap, decay_shift, head_gain, conv_taps, conv_gain, out_rec, out_conv):
    normed = layer_norm(tokens, norm_gain).astype(jnp.bfloat16)

    def project(weight):
        return jnp.dot(normed, weight, preferred_element_type=jnp.float32).astype(jnp.bfloat16)
    query_raw = project(w_query)
    forget_raw = project(w_forget)
    value_raw = project(w_value)
    rgate_raw = project(w_rgate)
    glu_value = project(w_glu_value)
    glu_gate = project(w_glu_gate)
    seq_len = tokens.shape[0]
    query = jax.nn.silu(query_raw.astype(jnp.float32)).reshape(seq_len, HEADS, HEAD)
    key_gate = forget_gap * jax.nn.sigmoid(-forget_raw.astype(jnp.float32))
    log_forget = jnp.log1p(-key_gate).reshape(seq_len, HEADS, HEAD) + decay_shift[:, :, None]
    values = value_raw.astype(jnp.float32).reshape(seq_len, HEADS, HEAD)
    recurrent_branch = block_scan(query, key_gate.reshape(seq_len, HEADS, HEAD), values, log_forget)
    recurrent_branch = recurrent_branch * lax.rsqrt(lax.optimization_barrier(jnp.mean(recurrent_branch * recurrent_branch, axis=-1, keepdims=True)) + head_epsilon) * head_gain
    rec_out = (recurrent_branch.reshape(seq_len, HEADS * HEAD) * jax.nn.silu(rgate_raw.astype(jnp.float32))).astype(jnp.bfloat16)
    mixed_in = (glu_value.astype(jnp.float32) * jax.nn.sigmoid(glu_gate.astype(jnp.float32))).astype(jnp.bfloat16)
    padded = lax.optimization_barrier(jnp.concatenate([jnp.zeros((CW - 1, DC), jnp.bfloat16), mixed_in], axis=0)).astype(jnp.float32)
    filtered = jnp.zeros((seq_len, DC), jnp.float32)
    for tap_index in range(CW):
        filtered = filtered + conv_taps[tap_index] * padded[tap_index:tap_index + seq_len]
    conv_out = jax.nn.silu(layer_norm(filtered, conv_gain)).astype(jnp.bfloat16)
    rec_share = HEADS * HEAD // N_TP
    conv_share = DC // N_TP
    mixed = jnp.zeros((seq_len, D), jnp.float32)
    for group in range(N_TP):
        term = jnp.dot(rec_out[:, group * rec_share:(group + 1) * rec_share], out_rec[group * rec_share:(group + 1) * rec_share], preferred_element_type=jnp.float32)
        term = term + jnp.dot(conv_out[:, group * conv_share:(group + 1) * conv_share], out_conv[group * conv_share:(group + 1) * conv_share], preferred_element_type=jnp.float32)
        mixed = mixed + lax.optimization_barrier(term.astype(jnp.bfloat16)).astype(jnp.float32)
    return mixed.astype(jnp.bfloat16)
```

```python
import functools

import jax
import jax.numpy as jnp
from jax import lax
from jax.experimental import pallas as pl
from jax.experimental.pallas import tpu as pltpu
from jax.sharding import PartitionSpec as P

CHUNK = 128
PAD = 16

norm_epsilon = 1e-05
head_epsilon = 1e-06


def dot(a, b, dims=((1,), (0,))):
    return lax.dot_general(a, b, (dims, ((), ())), preferred_element_type=jnp.float32)


def from_behind(value, axis, steps):
    count = lax.axis_size(axis)
    first, last = (max(0, -steps), min(count, count - steps))
    return lax.ppermute(value, axis, [(source, source + steps) for source in range(first, last)])


def layer_norm(values, gain):
    widened = values.astype(jnp.float32)
    row_mean = jnp.mean(widened, axis=-1, keepdims=True)
    centred = widened - row_mean
    row_var = jnp.mean(centred * centred, axis=-1, keepdims=True)
    return centred * lax.rsqrt(row_var + norm_epsilon) * gain


def scan_kernel(
    head, q_ref, f_ref, v_ref, gap_ref, shift_ref, near_ref, far_ref, pack_ref, state, offset
):
    step = pl.program_id(0)
    rows, width = q_ref.shape

    @pl.when(step == 0)
    def _():
        state[...] = jnp.zeros_like(state)
        offset[...] = jnp.zeros_like(offset)

    row = lax.broadcasted_iota(jnp.int32, (rows, rows), 0)
    col = lax.broadcasted_iota(jnp.int32, (rows, rows), 1)
    causal = row >= col
    lower = jnp.where(causal, 1.0, 0.0).astype(jnp.bfloat16)
    for h in range(width // head):
        part = slice(h * head, (h + 1) * head)
        query = q_ref[:, part].astype(jnp.float32)
        query = query * jax.nn.sigmoid(query)
        key = gap_ref[:, part] * jax.nn.sigmoid(-f_ref[:, part].astype(jnp.float32))
        log = jnp.log1p(-key) + shift_ref[:, h : h + 1]
        value = v_ref[:, part]
        high = log.astype(jnp.bfloat16)
        low = (log - high.astype(jnp.float32)).astype(jnp.bfloat16)
        total = dot(lower, high) + dot(lower, low)
        closing = total[rows - 1 : rows, :]
        middle = total[rows // 2 - 1 : rows // 2, :]
        query_mid = (query * jnp.exp(total - middle)).astype(jnp.bfloat16)
        key_mid = (key * jnp.exp(middle - total)).astype(jnp.bfloat16)
        scores = jnp.where(causal, dot(query_mid, key_mid, ((1,), (1,))), 0.0)
        query_near = query * jnp.exp(total)
        held = state[h]
        near_ref[:, part] = dot(scores.astype(jnp.bfloat16), value) + dot(
            query_near.astype(jnp.bfloat16), held.astype(jnp.bfloat16), ((1,), (1,))
        )
        far_ref[:, part] = (query_near * jnp.exp(offset[:, part])).astype(jnp.bfloat16)
        key_end = (key * jnp.exp(closing - total)).astype(jnp.bfloat16)
        state[h] = held * jnp.exp(closing) + dot(value, key_end, ((0,), (0,)))
        offset[:, part] = offset[:, part] + closing

    @pl.when(step == pl.num_programs(0) - 1)
    def _():
        place = lax.broadcasted_iota(jnp.int32, (PAD, head), 0)
        for h in range(width // head):
            pack_ref[h, 0:head, :] = state[h].astype(jnp.bfloat16)
            log = offset[:, h * head : (h + 1) * head]
            high = log.astype(jnp.bfloat16).astype(jnp.float32)
            rest = log - high
            mid = rest.astype(jnp.bfloat16).astype(jnp.float32)
            low = rest - mid
            tail = jnp.where(place == 0, high, jnp.where(place == 1, mid, jnp.where(place == 2, low, 0.0)))
            pack_ref[h, head : head + PAD, :] = tail.astype(jnp.bfloat16)


def local_scan(query_raw, forget_raw, value_raw, forget_gap, decay_shift, head):
    rows, width = query_raw.shape
    heads = width // head
    by_row = pl.BlockSpec((CHUNK, width), lambda i: (i, 0))
    whole = lambda shape: pl.BlockSpec(shape, lambda i: (0,) * len(shape))
    return pl.pallas_call(
        functools.partial(scan_kernel, head),
        grid=(rows // CHUNK,),
        in_specs=[
            by_row,
            by_row,
            by_row,
            whole((1, width)),
            pl.BlockSpec((CHUNK, heads), lambda i: (i, 0)),
        ],
        out_specs=[by_row, by_row, whole((heads, head + PAD, head))],
        out_shape=[
            jax.ShapeDtypeStruct((rows, width), jnp.float32),
            jax.ShapeDtypeStruct((rows, width), jnp.bfloat16),
            jax.ShapeDtypeStruct((heads, head + PAD, head), jnp.bfloat16),
        ],
        scratch_shapes=[
            pltpu.VMEM((heads, head, head), jnp.float32),
            pltpu.VMEM((1, width), jnp.float32),
        ],
        compiler_params=pltpu.CompilerParams(dimension_semantics=("arbitrary",)),
        cost_estimate=pl.CostEstimate(
            flops=rows * width * head * 12, bytes_accessed=rows * width * 12, transcendentals=rows * width * 8
        ),
    )(query_raw, forget_raw, value_raw, forget_gap[None], decay_shift)


def arrive(gathered_ref, arriving, head):
    me = lax.axis_index("sp")
    for h in range(arriving.shape[0]):
        arriving_h = jnp.zeros((head, head), jnp.float32)
        for d in range(gathered_ref.shape[0]):
            tail = gathered_ref[d, h, head : head + PAD, :].astype(jnp.float32)
            log = tail[0:1] + tail[1:2] + tail[2:3]
            stepped = arriving_h * jnp.exp(log) + gathered_ref[d, h, 0:head, :].astype(jnp.float32)
            arriving_h = jnp.where(d < me, stepped, arriving_h)
        arriving[h] = arriving_h.astype(jnp.bfloat16)


def finish_rows(head, channels, near, far, rgate, arriving, filtered, row_sum, row_square, conv_gain, head_gain):
    pieces = []
    for h in range(near.shape[1] // head):
        part = slice(h * head, (h + 1) * head)
        rec = near[:, part] + dot(far[:, part], arriving[h], ((1,), (1,)))
        rec = rec * lax.rsqrt(jnp.mean(rec * rec, axis=-1, keepdims=True) + head_epsilon) * head_gain
        gate = rgate[:, part].astype(jnp.float32)
        pieces.append((rec * (gate * jax.nn.sigmoid(gate))).astype(jnp.bfloat16))
    row_mean = row_sum / channels
    row_var = row_square / channels - row_mean * row_mean
    normed = (filtered - row_mean) * lax.rsqrt(row_var + norm_epsilon) * conv_gain
    return jnp.concatenate(pieces, axis=1), (normed * jax.nn.sigmoid(normed)).astype(jnp.bfloat16)


def finish_kernel(
    head, channels, near_ref, far_ref, rgate_ref, gathered_ref, filtered_ref, sum_ref, square_ref,
    conv_gain_ref, head_gain_ref, out_rec_ref, out_conv_ref, out_ref, arriving
):
    @pl.when(pl.program_id(0) == 0)
    def _():
        arrive(gathered_ref, arriving, head)

    rec, conv = finish_rows(
        head, channels, near_ref[...], far_ref[...], rgate_ref[...], arriving, filtered_ref[...],
        sum_ref[...], square_ref[...], conv_gain_ref[...], head_gain_ref[...],
    )
    out_ref[...] = (dot(rec, out_rec_ref[...]) + dot(conv, out_conv_ref[...])).astype(jnp.bfloat16)


def finish(near, far, rgate, gathered, filtered, row_sum, row_square, conv_gain, head_gain, out_rec, out_conv):
    rows, width = near.shape
    heads, head = gathered.shape[1], gathered.shape[3]
    columns = out_rec.shape[1]
    channels = filtered.shape[1] * lax.axis_size("tp")
    tile = min(256, rows)
    by_row = pl.BlockSpec((tile, width), lambda i: (i, 0))
    one = pl.BlockSpec((tile, 1), lambda i: (i, 0))
    whole = lambda shape: pl.BlockSpec(shape, lambda i: (0,) * len(shape))
    return pl.pallas_call(
        functools.partial(finish_kernel, head, channels),
        grid=(rows // tile,),
        in_specs=[
            by_row, by_row, by_row, whole(gathered.shape),
            pl.BlockSpec((tile, filtered.shape[1]), lambda i: (i, 0)), one, one,
            whole((1, filtered.shape[1])), whole((1, head)), whole(out_rec.shape), whole(out_conv.shape),
        ],
        out_specs=pl.BlockSpec((tile, columns), lambda i: (i, 0)),
        out_shape=jax.ShapeDtypeStruct((rows, columns), jnp.bfloat16),
        scratch_shapes=[pltpu.VMEM((heads, head, head), jnp.bfloat16)],
        compiler_params=pltpu.CompilerParams(dimension_semantics=("arbitrary",)),
    )(near, far, rgate, gathered, filtered, row_sum, row_square, conv_gain[None], head_gain[None], out_rec, out_conv)


def convolve(glu_value, glu_gate, conv_taps):
    row_count = glu_value.shape[0]
    mixed_in = (
        glu_value.astype(jnp.float32) * jax.nn.sigmoid(glu_gate.astype(jnp.float32))
    ).astype(jnp.bfloat16)
    reach = conv_taps.shape[0] - 1
    rim = from_behind(mixed_in[row_count - reach :], "sp", 1)
    padded = lax.optimization_barrier(jnp.concatenate([rim, mixed_in], axis=0)).astype(jnp.float32)
    filtered = jnp.zeros(glu_value.shape, jnp.float32)
    for tap_index in range(reach + 1):
        filtered = filtered + conv_taps[tap_index] * padded[tap_index : tap_index + row_count]
    row_sum, row_square = lax.psum(
        (jnp.sum(filtered, axis=1), jnp.sum(filtered * filtered, axis=1)), "tp"
    )
    return filtered, row_sum[:, None], row_square[:, None]


def on_device(
    tokens, norm_gain, w_query, w_forget, w_value, w_rgate, w_glu_value, w_glu_gate, forget_gap,
    decay_shift, head_gain, conv_taps, conv_gain, out_rec, out_conv,
):
    normed = layer_norm(tokens, norm_gain).astype(jnp.bfloat16)
    normed = lax.all_gather(normed, "tp", axis=0, tiled=True)

    def project(weight):
        return jnp.dot(normed, weight, preferred_element_type=jnp.float32).astype(jnp.bfloat16)

    near, far, pack = local_scan(
        project(w_query), project(w_forget), project(w_value), forget_gap, decay_shift, head_gain.shape[0]
    )
    gathered = lax.all_gather(pack[None], "sp", axis=0, tiled=True)
    filtered, row_sum, row_square = convolve(project(w_glu_value), project(w_glu_gate), conv_taps)
    partial = finish(
        near, far, project(w_rgate), gathered, filtered, row_sum, row_square, conv_gain, head_gain, out_rec, out_conv
    )
    return lax.psum_scatter(partial, "tp", scatter_dimension=0, tiled=True)


def solution(mesh):
    placed = (
        P(("sp", "tp"), None),
        P(),
        P(None, "tp"),
        P(None, "tp"),
        P(None, "tp"),
        P(None, "tp"),
        P(None, "tp"),
        P(None, "tp"),
        P("tp"),
        P("sp", "tp"),
        P(),
        P(None, "tp"),
        P("tp"),
        P("tp", None),
        P("tp", None),
    )
    return jax.shard_map(
        on_device, mesh=mesh, in_specs=placed, out_specs=P(("sp", "tp"), None), check_vma=False
    )
```

```python
import functools

import jax
import jax.numpy as jnp
from jax import lax
from jax.experimental import pallas as pl
from jax.experimental.pallas import tpu as pltpu
from jax.sharding import PartitionSpec as P

CHUNK = 128
PAD = 16
PIECES = 2
MESH = pl.DeviceIdType.MESH

norm_epsilon = 1e-05
head_epsilon = 1e-06


def dot(a, b, dims=((1,), (0,))):
    return lax.dot_general(a, b, (dims, ((), ())), preferred_element_type=jnp.float32)


def from_behind(value, axis, steps):
    count = lax.axis_size(axis)
    first, last = (max(0, -steps), min(count, count - steps))
    return lax.ppermute(value, axis, [(source, source + steps) for source in range(first, last)])


def layer_norm(values, gain):
    widened = values.astype(jnp.float32)
    row_mean = jnp.mean(widened, axis=-1, keepdims=True)
    centred = widened - row_mean
    row_var = jnp.mean(centred * centred, axis=-1, keepdims=True)
    return centred * lax.rsqrt(row_var + norm_epsilon) * gain


def partners():
    me = lax.axis_index("tp")
    pair = me + 1 - 2 * lax.rem(me, 2)
    return pair, lax.rem(me + 2, 4), lax.rem(pair + 2, 4), me


def greet(*others):
    barrier = pltpu.get_barrier_semaphore()
    for other in others:
        pl.semaphore_signal(barrier, inc=1, device_id={"tp": other}, device_id_type=MESH)
    pl.semaphore_wait(barrier, len(others))


def project_kernel(
    tokens_ref, gain_ref, w0, w1, w2, w3, w4, w5, out_ref,
    held, normed, weight, out, weight_sem, send_sem, recv_sem, out_sem,
):
    fetched = [pltpu.make_async_copy(w, weight.at[i], weight_sem.at[i]) for i, w in enumerate((w0, w1, w2, w3, w4, w5))]
    for one in fetched:
        one.start()
    pair, cross, diag, me = partners()
    greet(pair, cross)
    block = tokens_ref.shape[0]
    piece = block // PIECES

    def copy(source, target, kind, p, device):
        return pltpu.make_async_remote_copy(
            src_ref=source, dst_ref=target, send_sem=send_sem.at[kind, p], recv_sem=recv_sem.at[kind, p],
            device_id={"tp": device}, device_id_type=MESH,
        )

    parts = [pl.ds(p * piece, piece) for p in range(PIECES)]
    crossing = [copy(tokens_ref.at[rows, :], held.at[1, rows, :], 0, p, cross) for p, rows in enumerate(parts)]
    nearby = [copy(tokens_ref.at[rows, :], held.at[0, rows, :], 1, p, pair) for p, rows in enumerate(parts)]
    handed = [copy(held.at[1, rows, :], held.at[2, rows, :], 2, p, pair) for p, rows in enumerate(parts)]
    for one in crossing + nearby:
        one.start()
    stores = []

    def project(values, owner, p):
        normed[...] = layer_norm(values, gain_ref[...]).astype(jnp.bfloat16)
        if not stores:
            for one in fetched:
                one.wait()
        rows = pl.ds(pl.multiple_of(owner * block + p * piece, piece), piece)

        def step(i, carry):
            out[i, rows, :] = dot(normed[...], weight[i]).astype(jnp.bfloat16)
            return carry

        lax.fori_loop(0, len(fetched), step, 0)
        store = pltpu.make_async_copy(out.at[:, rows, :], out_ref.at[:, rows, :], out_sem.at[len(stores)])
        store.start()
        stores.append(store)

    for p, rows in enumerate(parts):
        project(tokens_ref[rows, :], me, p)
    for p, rows in enumerate(parts):
        nearby[p].wait_recv()
        project(held[0, rows, :], pair, p)
    for p, rows in enumerate(parts):
        crossing[p].wait_recv()
        handed[p].start()
        project(held[1, rows, :], cross, p)
        handed[p].wait_recv()
        project(held[2, rows, :], diag, p)
    for one in crossing + nearby + handed:
        one.wait_send()
    for one in stores:
        one.wait()


def gather_project(tokens, norm_gain, weights):
    block, depth = tokens.shape
    columns = weights[0].shape[1]
    rows = block * lax.axis_size("tp")
    count = len(weights)
    return pl.pallas_call(
        project_kernel,
        in_specs=[pl.BlockSpec(memory_space=pltpu.VMEM)] * 2 + [pl.BlockSpec(memory_space=pl.ANY)] * count,
        out_specs=pl.BlockSpec(memory_space=pl.ANY),
        out_shape=jax.ShapeDtypeStruct((count, rows, columns), jnp.bfloat16),
        scratch_shapes=[
            pltpu.VMEM((3, block, depth), jnp.bfloat16),
            pltpu.VMEM((block // PIECES, depth), jnp.bfloat16),
            pltpu.VMEM((count, depth, columns), jnp.bfloat16),
            pltpu.VMEM((count, rows, columns), jnp.bfloat16),
            pltpu.SemaphoreType.DMA((count,)),
            pltpu.SemaphoreType.DMA((3, PIECES)),
            pltpu.SemaphoreType.DMA((3, PIECES)),
            pltpu.SemaphoreType.DMA((4 * PIECES,)),
        ],
        compiler_params=pltpu.CompilerParams(
            collective_id=0, has_side_effects=True, vmem_limit_bytes=60000 * 1024
        ),
    )(tokens, norm_gain[None], *weights)


def scan_kernel(
    head, q_ref, f_ref, v_ref, gap_ref, shift_ref, near_ref, far_ref, pack_ref, state, offset
):
    step = pl.program_id(0)
    rows, width = q_ref.shape

    @pl.when(step == 0)
    def _():
        state[...] = jnp.zeros_like(state)
        offset[...] = jnp.zeros_like(offset)

    row = lax.broadcasted_iota(jnp.int32, (rows, rows), 0)
    col = lax.broadcasted_iota(jnp.int32, (rows, rows), 1)
    causal = row >= col
    lower = jnp.where(causal, 1.0, 0.0).astype(jnp.bfloat16)
    for h in range(width // head):
        part = slice(h * head, (h + 1) * head)
        query = q_ref[:, part].astype(jnp.float32)
        query = query * jax.nn.sigmoid(query)
        key = gap_ref[:, part] * jax.nn.sigmoid(-f_ref[:, part].astype(jnp.float32))
        log = jnp.log1p(-key) + shift_ref[:, h : h + 1]
        value = v_ref[:, part]
        high = log.astype(jnp.bfloat16)
        low = (log - high.astype(jnp.float32)).astype(jnp.bfloat16)
        total = dot(lower, high) + dot(lower, low)
        closing = total[rows - 1 : rows, :]
        middle = total[rows // 2 - 1 : rows // 2, :]
        query_mid = (query * jnp.exp(total - middle)).astype(jnp.bfloat16)
        key_mid = (key * jnp.exp(middle - total)).astype(jnp.bfloat16)
        scores = jnp.where(causal, dot(query_mid, key_mid, ((1,), (1,))), 0.0)
        query_near = query * jnp.exp(total)
        held = state[h]
        near_ref[:, part] = dot(scores.astype(jnp.bfloat16), value) + dot(
            query_near.astype(jnp.bfloat16), held.astype(jnp.bfloat16), ((1,), (1,))
        )
        far_ref[:, part] = (query_near * jnp.exp(offset[:, part])).astype(jnp.bfloat16)
        key_end = (key * jnp.exp(closing - total)).astype(jnp.bfloat16)
        state[h] = held * jnp.exp(closing) + dot(value, key_end, ((0,), (0,)))
        offset[:, part] = offset[:, part] + closing

    @pl.when(step == pl.num_programs(0) - 1)
    def _():
        place = lax.broadcasted_iota(jnp.int32, (PAD, head), 0)
        for h in range(width // head):
            pack_ref[h, 0:head, :] = state[h].astype(jnp.bfloat16)
            log = offset[:, h * head : (h + 1) * head]
            high = log.astype(jnp.bfloat16).astype(jnp.float32)
            rest = log - high
            mid = rest.astype(jnp.bfloat16).astype(jnp.float32)
            low = rest - mid
            tail = jnp.where(place == 0, high, jnp.where(place == 1, mid, jnp.where(place == 2, low, 0.0)))
            pack_ref[h, head : head + PAD, :] = tail.astype(jnp.bfloat16)


def local_scan(projected, forget_gap, decay_shift, head):
    rows, width = projected.shape[1:]
    heads = width // head

    def of(which):
        return pl.BlockSpec((None, CHUNK, width), lambda i: (which, i, 0))

    by_row = pl.BlockSpec((CHUNK, width), lambda i: (i, 0))
    whole = lambda shape: pl.BlockSpec(shape, lambda i: (0,) * len(shape))
    return pl.pallas_call(
        functools.partial(scan_kernel, head),
        grid=(rows // CHUNK,),
        in_specs=[
            of(0),
            of(1),
            of(2),
            whole((1, width)),
            pl.BlockSpec((CHUNK, heads), lambda i: (i, 0)),
        ],
        out_specs=[by_row, by_row, whole((heads, head + PAD, head))],
        out_shape=[
            jax.ShapeDtypeStruct((rows, width), jnp.float32),
            jax.ShapeDtypeStruct((rows, width), jnp.bfloat16),
            jax.ShapeDtypeStruct((heads, head + PAD, head), jnp.bfloat16),
        ],
        scratch_shapes=[
            pltpu.VMEM((heads, head, head), jnp.float32),
            pltpu.VMEM((1, width), jnp.float32),
        ],
        compiler_params=pltpu.CompilerParams(dimension_semantics=("arbitrary",)),
        cost_estimate=pl.CostEstimate(
            flops=rows * width * head * 12, bytes_accessed=rows * width * 12, transcendentals=rows * width * 8
        ),
    )(projected, projected, projected, forget_gap[None], decay_shift)


def arrive(gathered_ref, arriving, head):
    me = lax.axis_index("sp")
    for h in range(arriving.shape[0]):
        arriving_h = jnp.zeros((head, head), jnp.float32)
        for d in range(gathered_ref.shape[0]):
            tail = gathered_ref[d, h, head : head + PAD, :].astype(jnp.float32)
            log = tail[0:1] + tail[1:2] + tail[2:3]
            stepped = arriving_h * jnp.exp(log) + gathered_ref[d, h, 0:head, :].astype(jnp.float32)
            arriving_h = jnp.where(d < me, stepped, arriving_h)
        arriving[h] = arriving_h.astype(jnp.bfloat16)


def finish_rows(head, channels, near, far, rgate, arriving, filtered, row_sum, row_square, conv_gain, head_gain):
    pieces = []
    for h in range(near.shape[1] // head):
        part = slice(h * head, (h + 1) * head)
        rec = near[:, part] + dot(far[:, part], arriving[h], ((1,), (1,)))
        rec = rec * lax.rsqrt(jnp.mean(rec * rec, axis=-1, keepdims=True) + head_epsilon) * head_gain
        gate = rgate[:, part].astype(jnp.float32)
        pieces.append((rec * (gate * jax.nn.sigmoid(gate))).astype(jnp.bfloat16))
    row_mean = row_sum / channels
    row_var = row_square / channels - row_mean * row_mean
    normed = (filtered - row_mean) * lax.rsqrt(row_var + norm_epsilon) * conv_gain
    return jnp.concatenate(pieces, axis=1), (normed * jax.nn.sigmoid(normed)).astype(jnp.bfloat16)


def finish_kernel(
    head, channels, near_ref, far_ref, rgate_ref, gathered_ref, filtered_ref, sum_ref, square_ref,
    conv_gain_ref, head_gain_ref, out_rec_ref, out_conv_ref, out_ref,
    arriving, to_pair, from_pair, to_cross, from_cross, mine, send_sem, recv_sem,
):
    pair, cross, diag, me = partners()
    greet(pair, cross)
    block = out_ref.shape[0]
    piece = block // PIECES
    arrive(gathered_ref, arriving, head)

    def partial(owner, p):
        rows = pl.ds(pl.multiple_of(owner * block + p * piece, piece), piece)
        rec, conv = finish_rows(
            head, channels, near_ref[rows, :], far_ref[rows, :], rgate_ref[rows, :], arriving, filtered_ref[rows, :],
            sum_ref[rows, :], square_ref[rows, :], conv_gain_ref[...], head_gain_ref[...],
        )
        return (dot(rec, out_rec_ref[...]) + dot(conv, out_conv_ref[...])).astype(jnp.bfloat16)

    def copy(source, target, kind, p, device):
        return pltpu.make_async_remote_copy(
            src_ref=source, dst_ref=target, send_sem=send_sem.at[kind, p], recv_sem=recv_sem.at[kind, p],
            device_id={"tp": device}, device_id_type=MESH,
        )

    started, crossing, nearby = [], [], []
    for p in range(PIECES):
        rows = pl.ds(p * piece, piece)
        to_pair[0, rows, :] = partial(diag, p)
        lent = copy(to_pair.at[0, rows, :], from_pair.at[0, rows, :], 0, p, pair)
        lent.start()
        own = partial(cross, p).astype(jnp.float32)
        lent.wait_recv()
        to_cross[rows, :] = (own + from_pair[0, rows, :].astype(jnp.float32)).astype(jnp.bfloat16)
        sent = copy(to_cross.at[rows, :], from_cross.at[rows, :], 1, p, cross)
        sent.start()
        started.append(lent)
        crossing.append(sent)
    for p in range(PIECES):
        rows = pl.ds(p * piece, piece)
        to_pair[1, rows, :] = partial(pair, p)
        lent = copy(to_pair.at[1, rows, :], from_pair.at[1, rows, :], 2, p, pair)
        lent.start()
        nearby.append(lent)
    for p in range(PIECES):
        mine[pl.ds(p * piece, piece), :] = partial(me, p).astype(jnp.float32)
    for p in range(PIECES):
        rows = pl.ds(p * piece, piece)
        nearby[p].wait_recv()
        mine[rows, :] = mine[rows, :] + from_pair[1, rows, :].astype(jnp.float32)
    for p in range(PIECES):
        rows = pl.ds(p * piece, piece)
        crossing[p].wait_recv()
        out_ref[rows, :] = (mine[rows, :] + from_cross[rows, :].astype(jnp.float32)).astype(jnp.bfloat16)
    for sent in started + crossing + nearby:
        sent.wait_send()


def finish(near, far, projected, gathered, filtered, row_sum, row_square, conv_gain, head_gain, out_rec, out_conv):
    rows, width = near.shape
    heads, head = gathered.shape[1], gathered.shape[3]
    columns = out_rec.shape[1]
    block = rows // lax.axis_size("tp")
    channels = filtered.shape[1] * lax.axis_size("tp")
    whole = lambda shape: pl.BlockSpec(shape, lambda i: (0,) * len(shape))
    return pl.pallas_call(
        functools.partial(finish_kernel, head, channels),
        grid=(1,),
        in_specs=[
            whole(near.shape), whole(far.shape),
            pl.BlockSpec((None, rows, width), lambda i: (3, 0, 0)),
            whole(gathered.shape), whole(filtered.shape), whole(row_sum.shape), whole(row_square.shape),
            whole((1, filtered.shape[1])), whole((1, head)), whole(out_rec.shape), whole(out_conv.shape),
        ],
        out_specs=whole((block, columns)),
        out_shape=jax.ShapeDtypeStruct((block, columns), jnp.bfloat16),
        scratch_shapes=[
            pltpu.VMEM((heads, head, head), jnp.bfloat16),
            pltpu.VMEM((2, block, columns), jnp.bfloat16),
            pltpu.VMEM((2, block, columns), jnp.bfloat16),
            pltpu.VMEM((block, columns), jnp.bfloat16),
            pltpu.VMEM((block, columns), jnp.bfloat16),
            pltpu.VMEM((block, columns), jnp.float32),
            pltpu.SemaphoreType.DMA((3, PIECES)),
            pltpu.SemaphoreType.DMA((3, PIECES)),
        ],
        compiler_params=pltpu.CompilerParams(
            dimension_semantics=("arbitrary",), collective_id=1, has_side_effects=True,
            vmem_limit_bytes=60000 * 1024,
        ),
    )(near, far, projected, gathered, filtered, row_sum, row_square, conv_gain[None], head_gain[None], out_rec, out_conv)


def convolve(glu_value, glu_gate, conv_taps):
    row_count = glu_value.shape[0]
    mixed_in = (
        glu_value.astype(jnp.float32) * jax.nn.sigmoid(glu_gate.astype(jnp.float32))
    ).astype(jnp.bfloat16)
    reach = conv_taps.shape[0] - 1
    rim = from_behind(mixed_in[row_count - reach :], "sp", 1)
    padded = lax.optimization_barrier(jnp.concatenate([rim, mixed_in], axis=0)).astype(jnp.float32)
    filtered = jnp.zeros(glu_value.shape, jnp.float32)
    for tap_index in range(reach + 1):
        filtered = filtered + conv_taps[tap_index] * padded[tap_index : tap_index + row_count]
    row_sum, row_square = lax.psum(
        (jnp.sum(filtered, axis=1), jnp.sum(filtered * filtered, axis=1)), "tp"
    )
    return filtered, row_sum[:, None], row_square[:, None]


def on_device(
    tokens, norm_gain, w_query, w_forget, w_value, w_rgate, w_glu_value, w_glu_gate, forget_gap,
    decay_shift, head_gain, conv_taps, conv_gain, out_rec, out_conv,
):
    weights = (w_query, w_forget, w_value, w_rgate, w_glu_value, w_glu_gate)
    projected = gather_project(tokens, norm_gain, weights)
    near, far, pack = local_scan(projected, forget_gap, decay_shift, head_gain.shape[0])
    gathered = lax.all_gather(pack[None], "sp", axis=0, tiled=True)
    filtered, row_sum, row_square = convolve(projected[4], projected[5], conv_taps)
    return finish(
        near, far, projected, gathered, filtered, row_sum, row_square, conv_gain, head_gain, out_rec, out_conv
    )


def solution(mesh):
    placed = (
        P(("sp", "tp"), None),
        P(),
        P(None, "tp"),
        P(None, "tp"),
        P(None, "tp"),
        P(None, "tp"),
        P(None, "tp"),
        P(None, "tp"),
        P("tp"),
        P("sp", "tp"),
        P(),
        P(None, "tp"),
        P("tp"),
        P("tp", None),
        P("tp", None),
    )
    return jax.shard_map(
        on_device, mesh=mesh, in_specs=placed, out_specs=P(("sp", "tp"), None), check_vma=False
    )
```

```python
import functools

import jax
import jax.numpy as jnp
from jax import lax
from jax.experimental import pallas as pl
from jax.experimental.pallas import tpu as pltpu
from jax.sharding import PartitionSpec as P

CHUNK = 128
PAD = 16
PIECES = 2
REACH = 32
TILE = 64
LANES = 128
MESH = pl.DeviceIdType.MESH

norm_epsilon = 1e-05
head_epsilon = 1e-06


def dot(a, b, dims=((1,), (0,))):
    return lax.dot_general(a, b, (dims, ((), ())), preferred_element_type=jnp.float32)


def layer_norm(values, gain):
    widened = values.astype(jnp.float32)
    row_mean = jnp.mean(widened, axis=-1, keepdims=True)
    centred = widened - row_mean
    row_var = jnp.mean(centred * centred, axis=-1, keepdims=True)
    return centred * lax.rsqrt(row_var + norm_epsilon) * gain


def partners():
    me = lax.axis_index("tp")
    pair = me + 1 - 2 * lax.rem(me, 2)
    return pair, lax.rem(me + 2, 4), lax.rem(pair + 2, 4), me


def greet(*others):
    barrier = pltpu.get_barrier_semaphore()
    for other in others:
        pl.semaphore_signal(barrier, inc=1, device_id={"tp": other}, device_id_type=MESH)
    pl.semaphore_wait(barrier, len(others))


def project_kernel(
    tokens_ref, gain_ref, w0, w1, w2, w3, w4, w5, out_ref,
    held, normed, weight, out, weight_sem, send_sem, recv_sem, out_sem,
):
    fetched = [pltpu.make_async_copy(w, weight.at[i], weight_sem.at[i]) for i, w in enumerate((w0, w1, w2, w3, w4, w5))]
    for one in fetched:
        one.start()
    pair, cross, diag, me = partners()
    greet(pair, cross)
    block = tokens_ref.shape[0]
    piece = block // PIECES

    def copy(source, target, kind, p, device):
        return pltpu.make_async_remote_copy(
            src_ref=source, dst_ref=target, send_sem=send_sem.at[kind, p], recv_sem=recv_sem.at[kind, p],
            device_id={"tp": device}, device_id_type=MESH,
        )

    parts = [pl.ds(p * piece, piece) for p in range(PIECES)]
    crossing = [copy(tokens_ref.at[rows, :], held.at[1, rows, :], 0, p, cross) for p, rows in enumerate(parts)]
    nearby = [copy(tokens_ref.at[rows, :], held.at[0, rows, :], 1, p, pair) for p, rows in enumerate(parts)]
    handed = [copy(held.at[1, rows, :], held.at[2, rows, :], 2, p, pair) for p, rows in enumerate(parts)]
    for one in crossing + nearby:
        one.start()
    stores = []

    def project(values, owner, p):
        normed[...] = layer_norm(values, gain_ref[...]).astype(jnp.bfloat16)
        if not stores:
            for one in fetched:
                one.wait()
        rows = pl.ds(pl.multiple_of(owner * block + p * piece, piece), piece)

        def step(i, carry):
            out[i, rows, :] = dot(normed[...], weight[i]).astype(jnp.bfloat16)
            return carry

        lax.fori_loop(0, len(fetched), step, 0)
        store = pltpu.make_async_copy(out.at[:, rows, :], out_ref.at[:, rows, :], out_sem.at[len(stores)])
        store.start()
        stores.append(store)

    for p, rows in enumerate(parts):
        project(tokens_ref[rows, :], me, p)
    for p, rows in enumerate(parts):
        nearby[p].wait_recv()
        project(held[0, rows, :], pair, p)
    for p, rows in enumerate(parts):
        crossing[p].wait_recv()
        handed[p].start()
        project(held[1, rows, :], cross, p)
        handed[p].wait_recv()
        project(held[2, rows, :], diag, p)
    for one in crossing + nearby + handed:
        one.wait_send()
    for one in stores:
        one.wait()


def gather_project(tokens, norm_gain, weights):
    block, depth = tokens.shape
    columns = weights[0].shape[1]
    rows = block * lax.axis_size("tp")
    count = len(weights)
    return pl.pallas_call(
        project_kernel,
        in_specs=[pl.BlockSpec(memory_space=pltpu.VMEM)] * 2 + [pl.BlockSpec(memory_space=pl.ANY)] * count,
        out_specs=pl.BlockSpec(memory_space=pl.ANY),
        out_shape=jax.ShapeDtypeStruct((count, rows, columns), jnp.bfloat16),
        scratch_shapes=[
            pltpu.VMEM((3, block, depth), jnp.bfloat16),
            pltpu.VMEM((block // PIECES, depth), jnp.bfloat16),
            pltpu.VMEM((count, depth, columns), jnp.bfloat16),
            pltpu.VMEM((count, rows, columns), jnp.bfloat16),
            pltpu.SemaphoreType.DMA((count,)),
            pltpu.SemaphoreType.DMA((3, PIECES)),
            pltpu.SemaphoreType.DMA((3, PIECES)),
            pltpu.SemaphoreType.DMA((4 * PIECES,)),
        ],
        compiler_params=pltpu.CompilerParams(
            collective_id=0, has_side_effects=True, vmem_limit_bytes=60000 * 1024
        ),
    )(tokens, norm_gain[None], *weights)


def scan_kernel(
    head, q_ref, f_ref, v_ref, gap_ref, shift_ref, near_ref, far_ref, pack_ref, state, offset
):
    step = pl.program_id(0)
    rows, width = q_ref.shape

    @pl.when(step == 0)
    def _():
        state[...] = jnp.zeros_like(state)
        offset[...] = jnp.zeros_like(offset)

    row = lax.broadcasted_iota(jnp.int32, (rows, rows), 0)
    col = lax.broadcasted_iota(jnp.int32, (rows, rows), 1)
    causal = row >= col
    lower = jnp.where(causal, 1.0, 0.0).astype(jnp.bfloat16)
    for h in range(width // head):
        part = slice(h * head, (h + 1) * head)
        query = q_ref[:, part].astype(jnp.float32)
        query = query * jax.nn.sigmoid(query)
        key = gap_ref[:, part] * jax.nn.sigmoid(-f_ref[:, part].astype(jnp.float32))
        log = jnp.log1p(-key) + shift_ref[:, h : h + 1]
        value = v_ref[:, part]
        high = log.astype(jnp.bfloat16)
        low = (log - high.astype(jnp.float32)).astype(jnp.bfloat16)
        total = dot(lower, high) + dot(lower, low)
        closing = total[rows - 1 : rows, :]
        middle = total[rows // 2 - 1 : rows // 2, :]
        query_mid = (query * jnp.exp(total - middle)).astype(jnp.bfloat16)
        key_mid = (key * jnp.exp(middle - total)).astype(jnp.bfloat16)
        scores = jnp.where(causal, dot(query_mid, key_mid, ((1,), (1,))), 0.0)
        query_near = query * jnp.exp(total)
        held = state[h]
        near_ref[:, part] = dot(scores.astype(jnp.bfloat16), value) + dot(
            query_near.astype(jnp.bfloat16), held.astype(jnp.bfloat16), ((1,), (1,))
        )
        far_ref[:, part] = (query_near * jnp.exp(offset[:, part])).astype(jnp.bfloat16)
        key_end = (key * jnp.exp(closing - total)).astype(jnp.bfloat16)
        state[h] = held * jnp.exp(closing) + dot(value, key_end, ((0,), (0,)))
        offset[:, part] = offset[:, part] + closing

    @pl.when(step == pl.num_programs(0) - 1)
    def _():
        place = lax.broadcasted_iota(jnp.int32, (PAD, head), 0)
        for h in range(width // head):
            pack_ref[h, 0:head, :] = state[h].astype(jnp.bfloat16)
            log = offset[:, h * head : (h + 1) * head]
            high = log.astype(jnp.bfloat16).astype(jnp.float32)
            rest = log - high
            mid = rest.astype(jnp.bfloat16).astype(jnp.float32)
            low = rest - mid
            tail = jnp.where(place == 0, high, jnp.where(place == 1, mid, jnp.where(place == 2, low, 0.0)))
            pack_ref[h, head : head + PAD, :] = tail.astype(jnp.bfloat16)


def local_scan(projected, forget_gap, decay_shift, head):
    rows, width = projected.shape[1:]
    heads = width // head

    def of(which):
        return pl.BlockSpec((None, CHUNK, width), lambda i: (which, i, 0))

    by_row = pl.BlockSpec((CHUNK, width), lambda i: (i, 0))
    whole = lambda shape: pl.BlockSpec(shape, lambda i: (0,) * len(shape))
    return pl.pallas_call(
        functools.partial(scan_kernel, head),
        grid=(rows // CHUNK,),
        in_specs=[
            of(0),
            of(1),
            of(2),
            whole((1, width)),
            pl.BlockSpec((CHUNK, heads), lambda i: (i, 0)),
        ],
        out_specs=[by_row, by_row, whole((heads, head + PAD, head))],
        out_shape=[
            jax.ShapeDtypeStruct((rows, width), jnp.float32),
            jax.ShapeDtypeStruct((rows, width), jnp.bfloat16),
            jax.ShapeDtypeStruct((heads, head + PAD, head), jnp.bfloat16),
        ],
        scratch_shapes=[
            pltpu.VMEM((heads, head, head), jnp.float32),
            pltpu.VMEM((1, width), jnp.float32),
        ],
        compiler_params=pltpu.CompilerParams(dimension_semantics=("arbitrary",)),
        cost_estimate=pl.CostEstimate(
            flops=rows * width * head * 12, bytes_accessed=rows * width * 12, transcendentals=rows * width * 8
        ),
    )(projected, projected, projected, forget_gap[None], decay_shift)


def exchange_kernel(
    head, pack_ref, glu_value_ref, glu_gate_ref, taps_ref, arriving_ref, filtered_ref, stats_ref,
    gathered, rim, padded, own_stats, other_stats, send_sem, recv_sem, rim_sem, stat_send, stat_recv,
):
    me, tp = lax.axis_index("sp"), lax.axis_index("tp")
    count, groups = gathered.shape[0] + 1, other_stats.shape[0] + 1
    rows, width = filtered_ref.shape
    taps = taps_ref.shape[0]
    barrier = pltpu.get_barrier_semaphore()
    for k in range(1, count):
        pl.semaphore_signal(barrier, inc=1, device_id={"sp": lax.rem(me + k, count)}, device_id_type=MESH)
    for k in range(1, groups):
        pl.semaphore_signal(barrier, inc=1, device_id={"tp": lax.rem(tp + k, groups)}, device_id_type=MESH)
    pl.semaphore_wait(barrier, count + groups - 2)

    def mix(at, size):
        gate = glu_gate_ref[pl.ds(at, size), :].astype(jnp.float32)
        value = glu_value_ref[pl.ds(at, size), :].astype(jnp.float32)
        return (value * jax.nn.sigmoid(gate)).astype(jnp.bfloat16)

    after = lax.rem(me + 1, count)
    rim[0] = mix(rows - REACH, REACH)
    edge = pltpu.make_async_remote_copy(
        src_ref=rim.at[0], dst_ref=rim.at[1], send_sem=rim_sem.at[0], recv_sem=rim_sem.at[1],
        device_id={"sp": after}, device_id_type=MESH,
    )
    states = [
        pltpu.make_async_remote_copy(
            src_ref=pack_ref, dst_ref=gathered.at[k - 1], send_sem=send_sem.at[k - 1], recv_sem=recv_sem.at[k - 1],
            device_id={"sp": lax.rem(me + k, count)}, device_id_type=MESH,
        )
        for k in range(1, count)
    ]
    edge.start()
    for k, state in enumerate(states, 1):
        pl.when(me + k < count)(state.start)

    def mix_tile(i, carry):
        at = pl.multiple_of(i * TILE, TILE)
        padded[pl.ds(pl.multiple_of(at + REACH, 16), TILE), :] = mix(at, TILE).astype(jnp.float32)
        return carry

    lax.fori_loop(0, rows // TILE, mix_tile, 0)
    edge.wait_recv()
    padded[0:REACH, :] = jnp.where(me > 0, rim[1].astype(jnp.float32), 0.0)

    pick = lax.broadcasted_iota(jnp.int32, (8, LANES), 0)
    first = jnp.where(pick == 0, 1.0, 0.0)
    second = jnp.where(pick == 1, 1.0, 0.0)
    skip = REACH - taps + 1

    def filter_tile(i, carry):
        at = pl.multiple_of(i * LANES, LANES)
        for sub in range(LANES // TILE):
            base = pl.multiple_of(at + sub * TILE, TILE)
            for g in range(width // LANES):
                lanes = slice(g * LANES, (g + 1) * LANES)
                window = padded[pl.ds(base, TILE + REACH), lanes]
                total = jnp.zeros((TILE, LANES), jnp.float32)
                for r in range(8):
                    mine = [j for j in range(taps) if (j + skip) % 8 == r]
                    held = window[r : mine[-1] + skip + TILE]
                    for j in mine:
                        start = j + skip - r
                        total = total + taps_ref[j : j + 1, lanes] * held[start : start + TILE]
                filtered_ref[pl.ds(base, TILE), lanes] = total
        sums = jnp.zeros((LANES, LANES), jnp.float32)
        squares = jnp.zeros((LANES, LANES), jnp.float32)
        for g in range(width // LANES):
            value = filtered_ref[pl.ds(at, LANES), g * LANES : (g + 1) * LANES]
            sums = sums + value
            squares = squares + value * value
        own_stats[:, pl.ds(at, LANES)] = exact(first, sums, ((1,), (1,))) + exact(second, squares, ((1,), (1,)))
        return carry

    lax.fori_loop(0, rows // LANES, filter_tile, 0)
    stats = [
        pltpu.make_async_remote_copy(
            src_ref=own_stats, dst_ref=other_stats.at[k - 1], send_sem=stat_send.at[k - 1],
            recv_sem=stat_recv.at[k - 1], device_id={"tp": lax.rem(tp + k, groups)}, device_id_type=MESH,
        )
        for k in range(1, groups)
    ]
    for one in stats:
        one.start()
    for k, state in enumerate(states, 1):
        pl.when(me >= k)(state.wait_recv)
    for h in range(arriving_ref.shape[0]):
        arriving = jnp.zeros((head, head), jnp.float32)
        for k in range(count - 1, 0, -1):
            tail = gathered[k - 1, h, head : head + PAD, :].astype(jnp.float32)
            log = tail[0:1] + tail[1:2] + tail[2:3]
            stepped = arriving * jnp.exp(log) + gathered[k - 1, h, 0:head, :].astype(jnp.float32)
            arriving = jnp.where(me >= k, stepped, arriving)
        arriving_ref[h] = arriving.astype(jnp.bfloat16)
    for one in stats:
        one.wait_recv()
    eye = jnp.where(pick == lax.broadcasted_iota(jnp.int32, (8, LANES), 1), 1.0, 0.0)

    def stats_tile(i, carry):
        at = pl.multiple_of(i * LANES, LANES)
        total = own_stats[:, pl.ds(at, LANES)]
        for k in range(groups - 1):
            total = total + other_stats[k, :, pl.ds(at, LANES)]
        stats_ref[pl.ds(at, LANES), :] = exact(total, eye, ((0,), (0,)))
        return carry

    lax.fori_loop(0, rows // LANES, stats_tile, 0)
    edge.wait_send()
    for k, state in enumerate(states, 1):
        pl.when(me + k < count)(state.wait_send)
    for one in stats:
        one.wait_send()


def exact(a, b, dims):
    return lax.dot_general(
        a, b, (dims, ((), ())), precision=lax.Precision.HIGHEST, preferred_element_type=jnp.float32
    )


def exchange(pack, projected, conv_taps):
    heads, _, head = pack.shape
    rows, width = projected.shape[1:]
    count, groups = lax.axis_size("sp"), lax.axis_size("tp")
    whole = lambda shape: pl.BlockSpec(shape, lambda i: (0,) * len(shape))
    return pl.pallas_call(
        functools.partial(exchange_kernel, head),
        grid=(1,),
        in_specs=[
            whole(pack.shape),
            pl.BlockSpec((None, rows, width), lambda i: (4, 0, 0)),
            pl.BlockSpec((None, rows, width), lambda i: (5, 0, 0)),
            whole(conv_taps.shape),
        ],
        out_specs=[whole((heads, head, head)), whole((rows, width)), whole((rows, LANES))],
        out_shape=[
            jax.ShapeDtypeStruct((heads, head, head), jnp.bfloat16),
            jax.ShapeDtypeStruct((rows, width), jnp.float32),
            jax.ShapeDtypeStruct((rows, LANES), jnp.float32),
        ],
        scratch_shapes=[
            pltpu.VMEM((count - 1,) + pack.shape, jnp.bfloat16),
            pltpu.VMEM((2, REACH, width), jnp.bfloat16),
            pltpu.VMEM((rows + REACH, width), jnp.float32),
            pltpu.VMEM((8, rows), jnp.float32),
            pltpu.VMEM((groups - 1, 8, rows), jnp.float32),
            pltpu.SemaphoreType.DMA((count - 1,)),
            pltpu.SemaphoreType.DMA((count - 1,)),
            pltpu.SemaphoreType.DMA((2,)),
            pltpu.SemaphoreType.DMA((groups - 1,)),
            pltpu.SemaphoreType.DMA((groups - 1,)),
        ],
        compiler_params=pltpu.CompilerParams(
            dimension_semantics=("arbitrary",), collective_id=2, has_side_effects=True,
            vmem_limit_bytes=60000 * 1024,
        ),
    )(pack, projected, projected, conv_taps)


def finish_rows(head, channels, near, far, rgate, arriving, filtered, row_sum, row_square, conv_gain, head_gain):
    pieces = []
    for h in range(near.shape[1] // head):
        part = slice(h * head, (h + 1) * head)
        rec = near[:, part] + dot(far[:, part], arriving[h], ((1,), (1,)))
        rec = rec * lax.rsqrt(jnp.mean(rec * rec, axis=-1, keepdims=True) + head_epsilon) * head_gain
        gate = rgate[:, part].astype(jnp.float32)
        pieces.append((rec * (gate * jax.nn.sigmoid(gate))).astype(jnp.bfloat16))
    row_mean = row_sum / channels
    row_var = row_square / channels - row_mean * row_mean
    normed = (filtered - row_mean) * lax.rsqrt(row_var + norm_epsilon) * conv_gain
    return jnp.concatenate(pieces, axis=1), (normed * jax.nn.sigmoid(normed)).astype(jnp.bfloat16)


def finish_kernel(
    head, channels, near_ref, far_ref, rgate_ref, arriving, filtered_ref, stats_ref,
    conv_gain_ref, head_gain_ref, out_rec_ref, out_conv_ref, out_ref,
    to_pair, from_pair, to_cross, from_cross, mine, send_sem, recv_sem,
):
    pair, cross, diag, me = partners()
    greet(pair, cross)
    block = out_ref.shape[0]
    piece = block // PIECES

    def partial(owner, p):
        rows = pl.ds(pl.multiple_of(owner * block + p * piece, piece), piece)
        rec, conv = finish_rows(
            head, channels, near_ref[rows, :], far_ref[rows, :], rgate_ref[rows, :], arriving, filtered_ref[rows, :],
            stats_ref[rows, 0:1], stats_ref[rows, 1:2], conv_gain_ref[...], head_gain_ref[...],
        )
        return (dot(rec, out_rec_ref[...]) + dot(conv, out_conv_ref[...])).astype(jnp.bfloat16)

    def copy(source, target, kind, p, device):
        return pltpu.make_async_remote_copy(
            src_ref=source, dst_ref=target, send_sem=send_sem.at[kind, p], recv_sem=recv_sem.at[kind, p],
            device_id={"tp": device}, device_id_type=MESH,
        )

    started, crossing, nearby = [], [], []
    for p in range(PIECES):
        rows = pl.ds(p * piece, piece)
        to_pair[0, rows, :] = partial(diag, p)
        lent = copy(to_pair.at[0, rows, :], from_pair.at[0, rows, :], 0, p, pair)
        lent.start()
        own = partial(cross, p).astype(jnp.float32)
        lent.wait_recv()
        to_cross[rows, :] = (own + from_pair[0, rows, :].astype(jnp.float32)).astype(jnp.bfloat16)
        sent = copy(to_cross.at[rows, :], from_cross.at[rows, :], 1, p, cross)
        sent.start()
        started.append(lent)
        crossing.append(sent)
    for p in range(PIECES):
        rows = pl.ds(p * piece, piece)
        to_pair[1, rows, :] = partial(pair, p)
        lent = copy(to_pair.at[1, rows, :], from_pair.at[1, rows, :], 2, p, pair)
        lent.start()
        nearby.append(lent)
    for p in range(PIECES):
        mine[pl.ds(p * piece, piece), :] = partial(me, p).astype(jnp.float32)
    for p in range(PIECES):
        rows = pl.ds(p * piece, piece)
        nearby[p].wait_recv()
        mine[rows, :] = mine[rows, :] + from_pair[1, rows, :].astype(jnp.float32)
    for p in range(PIECES):
        rows = pl.ds(p * piece, piece)
        crossing[p].wait_recv()
        out_ref[rows, :] = (mine[rows, :] + from_cross[rows, :].astype(jnp.float32)).astype(jnp.bfloat16)
    for sent in started + crossing + nearby:
        sent.wait_send()


def finish(near, far, projected, arriving, filtered, stats, conv_gain, head_gain, out_rec, out_conv):
    rows, width = near.shape
    head = arriving.shape[2]
    columns = out_rec.shape[1]
    block = rows // lax.axis_size("tp")
    channels = filtered.shape[1] * lax.axis_size("tp")
    whole = lambda shape: pl.BlockSpec(shape, lambda i: (0,) * len(shape))
    return pl.pallas_call(
        functools.partial(finish_kernel, head, channels),
        grid=(1,),
        in_specs=[
            whole(near.shape), whole(far.shape),
            pl.BlockSpec((None, rows, width), lambda i: (3, 0, 0)),
            whole(arriving.shape), whole(filtered.shape), whole(stats.shape),
            whole((1, filtered.shape[1])), whole((1, head)), whole(out_rec.shape), whole(out_conv.shape),
        ],
        out_specs=whole((block, columns)),
        out_shape=jax.ShapeDtypeStruct((block, columns), jnp.bfloat16),
        scratch_shapes=[
            pltpu.VMEM((2, block, columns), jnp.bfloat16),
            pltpu.VMEM((2, block, columns), jnp.bfloat16),
            pltpu.VMEM((block, columns), jnp.bfloat16),
            pltpu.VMEM((block, columns), jnp.bfloat16),
            pltpu.VMEM((block, columns), jnp.float32),
            pltpu.SemaphoreType.DMA((3, PIECES)),
            pltpu.SemaphoreType.DMA((3, PIECES)),
        ],
        compiler_params=pltpu.CompilerParams(
            dimension_semantics=("arbitrary",), collective_id=1, has_side_effects=True,
            vmem_limit_bytes=60000 * 1024,
        ),
    )(near, far, projected, arriving, filtered, stats, conv_gain[None], head_gain[None], out_rec, out_conv)


def on_device(
    tokens, norm_gain, w_query, w_forget, w_value, w_rgate, w_glu_value, w_glu_gate, forget_gap,
    decay_shift, head_gain, conv_taps, conv_gain, out_rec, out_conv,
):
    weights = (w_query, w_forget, w_value, w_rgate, w_glu_value, w_glu_gate)
    projected = gather_project(tokens, norm_gain, weights)
    near, far, pack = local_scan(projected, forget_gap, decay_shift, head_gain.shape[0])
    arriving, filtered, stats = exchange(pack, projected, conv_taps)
    return finish(
        near, far, projected, arriving, filtered, stats, conv_gain, head_gain, out_rec, out_conv
    )


def solution(mesh):
    placed = (
        P(("sp", "tp"), None),
        P(),
        P(None, "tp"),
        P(None, "tp"),
        P(None, "tp"),
        P(None, "tp"),
        P(None, "tp"),
        P(None, "tp"),
        P("tp"),
        P("sp", "tp"),
        P(),
        P(None, "tp"),
        P("tp"),
        P("tp", None),
        P("tp", None),
    )
    return jax.shard_map(
        on_device, mesh=mesh, in_specs=placed, out_specs=P(("sp", "tp"), None), check_vma=False
    )
```
